32 devices in a mesh: grp: 2 (over x), tp: 4 (over y, core), dp: 4 (over z).
Axes of the slice: x: 2, y: 2, z: 4, core: 2. Of those that a mesh axis runs over, the one named last changes fastest.
Arguments:
- hidden_in: bfloat16 [256, 4096], P('grp', 'dp'), parts along dimension 0, may hold values from -6 to 6
- state_in: float32 [2, 256, 32, 4096], P(None, ('grp', 'dp'), 'tp'), parts along dimension 1, may hold values from -0.6 to 0.6
- w_query: bfloat16 [2, 4096, 2048], P(None, 'dp', 'tp'), may hold values from -0.09375 to 0.09375
- w_key: bfloat16 [2, 4096, 2048], P(None, 'dp', 'tp'), may hold values from -0.09375 to 0.09375
- w_value: bfloat16 [2, 4096, 2048], P(None, 'dp', 'tp'), may hold values from -0.09375 to 0.09375
- w_gate: bfloat16 [2, 4096, 2048], P(None, 'dp', 'tp'), may hold values from -0.09375 to 0.09375
- w_beta: bfloat16 [2, 4096, 32], P(None, 'dp'), may hold values from -0.09375 to 0.09375
- w_decay: bfloat16 [2, 4096, 32], P(None, 'dp'), may hold values from -0.09375 to 0.09375
- decay_rate: float32 [2, 32], P(None, 'tp'), may hold values from 0.05 to 2
- out_gain: float32 [2, 64], replicated, may hold values from 0.1 to 1.9
- w_out: bfloat16 [2, 2048, 4096], P(None, 'tp', 'dp'), may hold values from -0.0625 to 0.0625
- post_gain: float32 [2, 4096], P(None, 'dp'), may hold values from 0.1 to 1.9
- post_bias: float32 [2, 4096], P(None, 'dp'), may hold values from -1.8 to 1.8
Outputs:
- hidden_out: bfloat16 [256, 4096], P('grp', 'dp'), parts along dimension 0
- state_out: float32 [2, 256, 32, 4096], P(None, ('grp', 'dp'), 'tp'), parts along dimension 1
The draws below stay inside these ranges and needn't reach their ends.
There are 2 independent parts, one for each index of `grp`. The reference program is written for one: setup_inputs(seed, part) draws one part's arguments, and reference() takes and returns one part's arrays. A program takes and returns all parts, laid end to end along the dimension named above; an argument that names none is the same for every part. Nothing has to cross between parts.
All inputs are finite; a program needn't handle non-finite values.
Results may differ from the reference program's by a relative error of at most 0.018.
Values may be sent and summed in bfloat16 or wider, within the bound.
A program may use at most 128 MiB of HBM per device.

```python
import math
import jax
import jax.numpy as jnp
from jax import lax

D = 4096
HEADS = 32
HEAD_DIM = 64
SEQS = 128
LAYERS = 2
N_DP = 4


def block_levels(stream_key, shape, pieces, smallest, high):
    gain = 1.0
    for dim, blocks in pieces:
        draws = jax.random.uniform(jax.random.fold_in(jax.random.fold_in(stream_key, 6), dim), (blocks,), jnp.float32, smallest / len(pieces), high / len(pieces))
        gain = gain * jnp.repeat(jnp.exp(draws), shape[dim] // blocks).reshape((-1,) + (1,) * (len(shape) - 1 - dim))
    return gain


def normal_values(own_key, dims, width, bound, pieces=(), dtype=jnp.bfloat16):
    drawn = width * jax.random.normal(own_key, dims, jnp.float32)
    if pieces:
        drawn = drawn * block_levels(own_key, dims, pieces, -0.22, 0.18)
    return jnp.clip(drawn, -bound, bound).astype(dtype)


def setup_inputs(seed: int = 0, part: int = 0) -> dict:
    key_of = jax.random.split(jax.random.key(seed), 14)
    part_keys = jax.random.split(jax.random.fold_in(key_of[13], part), 14)
    return {
        "hidden_in": normal_values(part_keys[0], (SEQS, D), 1.0, 6.0, ((1, 4),)),
        "state_in": normal_values(part_keys[1], (LAYERS, SEQS, HEADS, HEAD_DIM * HEAD_DIM), 0.1, 0.6, ((1, 4), (2, 4)), jnp.float32),
        "w_query": normal_values(key_of[2], (LAYERS, D, HEADS * HEAD_DIM), D ** -0.5, 0.09375, ((1, 4), (2, 4))),
        "w_key": normal_values(key_of[3], (LAYERS, D, HEADS * HEAD_DIM), D ** -0.5, 0.09375, ((1, 4), (2, 4))),
        "w_value": normal_values(key_of[4], (LAYERS, D, HEADS * HEAD_DIM), D ** -0.5, 0.09375, ((1, 4), (2, 4))),
        "w_gate": normal_values(key_of[5], (LAYERS, D, HEADS * HEAD_DIM), D ** -0.5, 0.09375, ((1, 4), (2, 4))),
        "w_beta": normal_values(key_of[6], (LAYERS, D, HEADS), D ** -0.5, 0.09375, ((1, 4),)),
        "w_decay": normal_values(key_of[7], (LAYERS, D, HEADS), D ** -0.5, 0.09375, ((1, 4),)),
        "decay_rate": jnp.clip(jnp.exp(math.log(2.0) - 3.6888794 * jax.random.uniform(key_of[8], (LAYERS, HEADS), jnp.float32) ** block_levels(key_of[8], (LAYERS, HEADS), ((1, 4),), -0.2, 0.2)), 0.05, 2.0),
        "out_gain": jnp.clip(1.0 + 0.18 * jax.random.normal(key_of[9], (LAYERS, HEAD_DIM), jnp.float32), 0.1, 1.9),
        "w_out": normal_values(key_of[10], (LAYERS, HEADS * HEAD_DIM, D), (4 * HEADS * HEAD_DIM) ** -0.5, 0.0625, ((1, 4), (2, 4))),
        "post_gain": jnp.clip(1.0 + 0.18 * jax.random.normal(key_of[11], (LAYERS, D), jnp.float32), 0.1, 1.9),
        "post_bias": normal_values(key_of[12], (LAYERS, D), 0.3, 1.8, ((1, 4),), jnp.float32),
    }


residual_scale = 2.0 ** 0.5

def unit_norm(tensor):
    return tensor * lax.rsqrt(lax.optimization_barrier(jnp.sum(tensor * tensor, axis=-1, keepdims=True)) + 1e-06)

def project(stream, weight):
    row_count = stream.shape[1] // N_DP
    blocked_x = stream.reshape(stream.shape[0], N_DP, row_count).astype(jnp.float32)
    blocked_w = weight.reshape(N_DP, row_count, weight.shape[1]).astype(jnp.float32)
    partials = jnp.einsum('bnd,nde->nbe', blocked_x, blocked_w).astype(jnp.bfloat16)
    return lax.optimization_barrier(jnp.sum(partials.astype(jnp.float32), axis=0)).astype(jnp.bfloat16)

def delta_step(state_now, query_pre, key_pre, value_pre, gate_pre, beta_pre, decay_pre, decay_speed, norm_gain):
    head_dim = query_pre.shape[-1]
    query_unit = unit_norm(query_pre.astype(jnp.float32)) * head_dim ** (-0.5)
    key_unit = unit_norm(key_pre.astype(jnp.float32))
    values_f = value_pre.astype(jnp.float32)
    beta_gate = jax.nn.sigmoid(beta_pre.astype(jnp.float32))[..., None, None]
    retain = jnp.exp(-decay_speed * jax.nn.softplus(decay_pre.astype(jnp.float32)))[..., None, None]
    matrix = state_now.reshape(state_now.shape[0], state_now.shape[1], head_dim, head_dim)
    readout = jnp.einsum('bhd,bhde->bhe', key_unit, matrix, precision=lax.Precision.HIGHEST)
    matrix = retain * (matrix - beta_gate * key_unit[..., :, None] * readout[..., None, :]) + beta_gate * key_unit[..., :, None] * values_f[..., None, :]
    output_vec = jnp.einsum('bhd,bhde->bhe', query_unit, matrix, precision=lax.Precision.HIGHEST)
    output_vec = output_vec * lax.rsqrt(lax.optimization_barrier(jnp.mean(output_vec * output_vec, axis=-1, keepdims=True)) + 1e-05)
    output_vec = output_vec * norm_gain * jax.nn.silu(gate_pre.astype(jnp.float32))
    return (matrix.reshape(state_now.shape), output_vec.astype(jnp.bfloat16))

def reference(hidden_in, state_in, w_query, w_key, w_value, w_gate, w_beta, w_decay, decay_rate, out_gain, w_out, post_gain, post_bias):
    stream = hidden_in
    states = []
    for block_index in range(LAYERS):
        shaped = (SEQS, HEADS, HEAD_DIM)
        query_pre = project(stream, w_query[block_index]).reshape(shaped)
        key_pre = project(stream, w_key[block_index]).reshape(shaped)
        value_pre = project(stream, w_value[block_index]).reshape(shaped)
        gate_pre = project(stream, w_gate[block_index]).reshape(shaped)
        beta_pre = project(stream, w_beta[block_index])
        decay_pre = project(stream, w_decay[block_index])
        new_state, read_vec = delta_step(state_in[block_index], query_pre, key_pre, value_pre, gate_pre, beta_pre, decay_pre, decay_rate[block_index][None, :], out_gain[block_index])
        states.append(new_state)
        mixed = jnp.dot(read_vec.reshape(SEQS, HEADS * HEAD_DIM), w_out[block_index], preferred_element_type=jnp.float32)
        combined = residual_scale * stream.astype(jnp.float32) + mixed
        mean_row = lax.optimization_barrier(jnp.mean(combined, axis=-1, keepdims=True))
        var_row = lax.optimization_barrier(jnp.mean(combined * combined, axis=-1, keepdims=True)) - mean_row * mean_row
        normed = (combined - mean_row) * lax.rsqrt(var_row + 1e-05)
        stream = (normed * post_gain[block_index] + post_bias[block_index]).astype(jnp.bfloat16)
    return (stream, jnp.stack(states, axis=0))
```

```python
import functools

import jax
import jax.numpy as jnp
from jax import lax
from jax.experimental import pallas as pl
from jax.experimental.pallas import tpu as pltpu
from jax.sharding import PartitionSpec as P

D = 4096
HEAD_DIM = 64
LAYERS = 2


residual_scale = 2.0**0.5


def unit_norm(tensor):
    return tensor * lax.rsqrt(jnp.sum(tensor * tensor, axis=-1, keepdims=True) + 1e-06)


def delta_step(
    state_now, query_pre, key_pre, value_pre, gate_pre, beta_pre, decay_pre, decay_speed, norm_gain
):
    head_dim = query_pre.shape[-1]
    query_unit = unit_norm(query_pre.astype(jnp.float32)) * head_dim ** (-0.5)
    key_unit = unit_norm(key_pre.astype(jnp.float32))
    values_f = value_pre.astype(jnp.float32)
    beta_gate = jax.nn.sigmoid(beta_pre.astype(jnp.float32))[..., None, None]
    retain = jnp.exp(-decay_speed * jax.nn.softplus(decay_pre.astype(jnp.float32)))[..., None, None]
    matrix = state_now.reshape(state_now.shape[0], state_now.shape[1], head_dim, head_dim)
    readout = jnp.einsum("bhd,bhde->bhe", key_unit, matrix, precision=lax.Precision.HIGHEST)
    matrix = (
        retain * (matrix - beta_gate * key_unit[..., :, None] * readout[..., None, :])
        + beta_gate * key_unit[..., :, None] * values_f[..., None, :]
    )
    output_vec = jnp.einsum("bhd,bhde->bhe", query_unit, matrix, precision=lax.Precision.HIGHEST)
    output_vec = output_vec * lax.rsqrt(
        jnp.mean(output_vec * output_vec, axis=-1, keepdims=True) + 1e-05
    )
    output_vec = output_vec * norm_gain * jax.nn.silu(gate_pre.astype(jnp.float32))
    return (matrix.reshape(state_now.shape), output_vec.astype(jnp.bfloat16))


def layer_norm(combined, totals, gain_row, bias_row):
    mean_row = (totals[0] / D)[:, None]
    var_row = (totals[1] / D)[:, None] - mean_row * mean_row
    normed = (combined - mean_row) * lax.rsqrt(var_row + 1e-05)
    return (normed * gain_row + bias_row).astype(jnp.bfloat16)


def per_device(
    hidden_in,
    state_in,
    w_query,
    w_key,
    w_value,
    w_gate,
    w_beta,
    w_decay,
    decay_rate,
    out_gain,
    w_out,
    post_gain,
    post_bias,
):
    stream = hidden_in
    states = []
    heads_here = w_query.shape[2] // HEAD_DIM
    first_head = lax.axis_index("tp") * heads_here
    for block_index in range(LAYERS):
        beta_cols = lax.dynamic_slice_in_dim(w_beta[block_index], first_head, heads_here, 1)
        decay_cols = lax.dynamic_slice_in_dim(w_decay[block_index], first_head, heads_here, 1)
        part_query = jnp.dot(stream, w_query[block_index], preferred_element_type=jnp.float32)
        part_key = jnp.dot(stream, w_key[block_index], preferred_element_type=jnp.float32)
        part_value = jnp.dot(stream, w_value[block_index], preferred_element_type=jnp.float32)
        part_gate = jnp.dot(stream, w_gate[block_index], preferred_element_type=jnp.float32)
        part_beta = jnp.dot(stream, beta_cols, preferred_element_type=jnp.float32)
        part_decay = jnp.dot(stream, decay_cols, preferred_element_type=jnp.float32)
        projected = (
            lax.psum_scatter(
                part_query.astype(jnp.bfloat16), "dp", scatter_dimension=0, tiled=True
            ).astype(jnp.float32),
            lax.psum_scatter(
                part_key.astype(jnp.bfloat16), "dp", scatter_dimension=0, tiled=True
            ).astype(jnp.float32),
            lax.psum_scatter(
                part_value.astype(jnp.bfloat16), "dp", scatter_dimension=0, tiled=True
            ).astype(jnp.float32),
            lax.psum_scatter(
                part_gate.astype(jnp.bfloat16), "dp", scatter_dimension=0, tiled=True
            ).astype(jnp.float32),
            lax.psum_scatter(
                part_beta.astype(jnp.bfloat16), "dp", scatter_dimension=0, tiled=True
            ).astype(jnp.float32),
            lax.psum_scatter(
                part_decay.astype(jnp.bfloat16), "dp", scatter_dimension=0, tiled=True
            ).astype(jnp.float32),
        )
        local_rows = projected[0].shape[0]
        shaped = (local_rows, heads_here, HEAD_DIM)
        query_pre = projected[0].astype(jnp.bfloat16).reshape(shaped)
        key_pre = projected[1].astype(jnp.bfloat16).reshape(shaped)
        value_pre = projected[2].astype(jnp.bfloat16).reshape(shaped)
        gate_pre = projected[3].astype(jnp.bfloat16).reshape(shaped)
        beta_pre = projected[4].astype(jnp.bfloat16)
        decay_pre = projected[5].astype(jnp.bfloat16)
        new_state, read_vec = delta_step(
            state_in[block_index],
            query_pre,
            key_pre,
            value_pre,
            gate_pre,
            beta_pre,
            decay_pre,
            decay_rate[block_index][None, :],
            out_gain[block_index],
        )
        states.append(new_state)
        read_flat = read_vec.reshape(local_rows, heads_here * HEAD_DIM)
        out_weight = w_out[block_index]
        gathered = lax.all_gather(read_flat, "dp", axis=0, tiled=True)
        share_rows = gathered.shape[0] // lax.axis_size("tp")
        mixed_sum = lax.psum_scatter(
            jnp.dot(gathered, out_weight, preferred_element_type=jnp.float32).astype(jnp.bfloat16),
            "tp",
            scatter_dimension=0,
            tiled=True,
        ).astype(jnp.float32)
        residual = lax.dynamic_slice_in_dim(
            stream, lax.axis_index("tp") * share_rows, share_rows, 0
        )
        combined = residual_scale * residual.astype(jnp.float32) + mixed_sum
        totals = lax.psum((jnp.sum(combined, axis=1), jnp.sum(combined * combined, axis=1)), "dp")
        normed_rows = layer_norm(combined, totals, post_gain[block_index], post_bias[block_index])
        stream = lax.all_gather(normed_rows, "tp", axis=0, tiled=True)
    return (stream, jnp.stack(states, axis=0))

MESH = pl.DeviceIdType.MESH
LANES = 128
F32 = jnp.float32
BF16 = jnp.bfloat16


def fused_kernel(
    n_dp,
    n_tp,
    hidden,
    state,
    w_query,
    w_key,
    w_value,
    w_gate,
    w_beta,
    w_decay,
    rate,
    gain,
    w_out,
    post_gain,
    post_bias,
    hidden_out,
    state_out,
    stream,
    st,
    wp,
    wbd,
    wo,
    psend,
    precv,
    bsend,
    brecv,
    ex,
    qkx,
    qk,
    vg,
    bt,
    dc,
    accq,
    acck,
    av,
    wv,
    rd,
    rall,
    msend,
    mrecv,
    ssend,
    srecv,
    load_sem,
    out_sem,
    p_ss,
    p_rs,
    r_ss,
    r_rs,
    m_ss,
    m_rs,
    s_ss,
    s_rs,
    g_ss,
    g_rs,
):
    layers, seqs, heads, flat = st.shape
    rows, feat = stream.shape[1:]
    cols = wo.shape[1]
    share = rows // n_tp
    all_heads = wbd.shape[3]
    hd = HEAD_DIM
    tiles = flat // LANES
    me_dp = lax.axis_index("dp")
    me_tp = lax.axis_index("tp")

    loads = {}

    def load(name, src, dst, layer, index):
        copy = pltpu.make_async_copy(src, dst, load_sem.at[layer, index])
        copy.start()
        loads[name, layer] = copy

    first = pltpu.make_async_copy(hidden, stream.at[0], load_sem.at[0, 8])
    first.start()
    projections = (w_key, w_query, w_value, w_gate)
    for layer in range(layers):
        for j, w in enumerate(projections):
            load(j, w.at[layer], wp.at[layer, j], layer, j)
        load("b", w_beta.at[layer], wbd.at[layer, 0], layer, 4)
        load("d", w_decay.at[layer], wbd.at[layer, 1], layer, 5)
        load("s", state.at[layer], st.at[layer], layer, 6)
        load("o", w_out.at[layer], wo.at[layer], layer, 7)

    barrier = pltpu.get_barrier_semaphore()
    for i in range(1, n_dp):
        pl.semaphore_signal(
            barrier, inc=1, device_id={"dp": lax.rem(me_dp + i, n_dp)}, device_id_type=MESH
        )
    for i in range(1, n_tp):
        pl.semaphore_signal(
            barrier, inc=1, device_id={"tp": lax.rem(me_tp + i, n_tp)}, device_id_type=MESH
        )

    chunk = 1024

    def fill(n, carry):
        at = pl.multiple_of(n * chunk, chunk)
        row = lax.broadcasted_iota(jnp.int32, (LANES, chunk), 0)
        col = lax.broadcasted_iota(jnp.int32, (LANES, chunk), 1) + at
        hit = jnp.logical_and(col >= row * hd, col < (row + 1) * hd)
        ex[:, pl.ds(at, chunk)] = jnp.where(hit, 1.0, 0.0).astype(BF16)
        return carry

    lax.fori_loop(0, 2 * flat // chunk, fill, 0)
    pl.semaphore_wait(barrier, n_dp - 1 + n_tp - 1)

    lane = lax.broadcasted_iota(jnp.int32, (seqs, LANES), 1)
    low = lane < hd
    lane_r = lax.broadcasted_iota(jnp.int32, (seqs * heads, LANES), 1)
    low_r = lane_r < hd

    def swap(x):
        return pltpu.roll(x, hd, 1)

    def to_rows(dst, a, b):
        for h in range(heads):
            sl = slice(h // 2 * LANES, h // 2 * LANES + LANES)
            at, bt_ = a[:, sl], b[:, sl]
            both = jnp.where(low, at, swap(bt_)) if h % 2 == 0 else jnp.where(low, swap(at), bt_)
            dst[pl.ds(h, seqs, stride=heads), :] = both

    sends = []

    def remote(src, dst, ss, rs, axis, peer):
        copy = pltpu.make_async_remote_copy(
            src_ref=src,
            dst_ref=dst,
            send_sem=ss,
            recv_sem=rs,
            device_id={axis: peer},
            device_id_type=MESH,
        )
        copy.start()
        sends.append(copy)
        return copy

    first.wait()
    gain_all = gain[...]
    for layer in range(layers):
        x = stream[layer]

        def scatter(group, src, dst):
            copies = []
            for i in range(1, n_dp):
                peer = lax.rem(me_dp + i, n_dp)
                copies.append(
                    remote(
                        src.at[pl.ds(pl.multiple_of(peer * seqs, seqs), seqs)],
                        dst.at[i - 1],
                        p_ss.at[layer, group, i - 1],
                        p_rs.at[layer, group, i - 1],
                        "dp",
                        peer,
                    )
                )
            return copies

        mine = pl.ds(pl.multiple_of(me_dp * seqs, seqs), seqs)
        scattered = []
        for j in range(4):
            loads[j, layer].wait()
            part = jnp.dot(x, wp[layer, j], preferred_element_type=F32)
            psend[layer, j] = part.astype(BF16)
            scattered.append(scatter(j, psend.at[layer, j], precv.at[layer, j]))
            if j == 1:
                loads["b", layer].wait()
                loads["d", layer].wait()
                pb = jnp.dot(x, wbd[layer, 0], preferred_element_type=F32)
                pd = jnp.dot(x, wbd[layer, 1], preferred_element_type=F32)
                pad = jnp.zeros((rows, LANES - 2 * all_heads), F32)
                bsend[layer] = jnp.concatenate([pb, pd, pad], axis=1).astype(BF16)
                scattered_b = scatter(4, bsend.at[layer], brecv.at[layer])

        def total(copies, own, got):
            acc = own.astype(F32)
            for i, copy in enumerate(copies):
                copy.wait_recv()
                acc = acc + got[i].astype(F32)
            return acc.astype(BF16).astype(F32)

        def projected(j):
            return total(scattered[j], psend[layer, j, mine, :], precv.at[layer, j])

        keys = projected(0)
        queries = projected(1)
        to_rows(qk, queries, keys)
        both = qk[...]
        both_b = both.astype(BF16)

        def expand(n, carry):
            at = pl.multiple_of(n * chunk, chunk)
            qkx[:, pl.ds(at, chunk)] = jnp.dot(
                both_b, ex[:, pl.ds(at, chunk)], preferred_element_type=F32
            )
            return carry

        lax.fori_loop(0, 2 * flat // chunk, expand, 0)
        loads["s", layer].wait()

        def reduce(s, carry):
            at = pl.ds(pl.multiple_of(s * heads, heads), heads)
            q_sums = [None, None]
            k_sums = [None, None]
            for t in range(tiles):
                sl = slice(t * LANES, (t + 1) * LANES)
                value = st[layer, s, :, sl]
                qp = qkx[at, sl] * value
                kp = qkx[at, flat + t * LANES : flat + (t + 1) * LANES] * value
                p = t % 2
                q_sums[p] = qp if q_sums[p] is None else q_sums[p] + qp
                k_sums[p] = kp if k_sums[p] is None else k_sums[p] + kp
            accq[at, :] = q_sums[0] + q_sums[1]
            acck[at, :] = k_sums[0] + k_sums[1]
            return carry

        lax.fori_loop(0, seqs, reduce, 0)

        bd = total(scattered_b, bsend[layer, mine, :], brecv.at[layer])
        for h in range(heads):
            head = me_tp * heads + h
            beta_h = jnp.sum(jnp.where(lane == head, bd, 0.0), axis=1, keepdims=True)
            decay_h = jnp.sum(jnp.where(lane == head + all_heads, bd, 0.0), axis=1, keepdims=True)
            soft = jnp.maximum(decay_h, 0.0) + jnp.log1p(jnp.exp(-jnp.abs(decay_h)))
            retain_h = jnp.exp(-rate[layer, h] * soft)
            bt[pl.ds(h, seqs, stride=heads), :] = jnp.broadcast_to(
                jax.nn.sigmoid(beta_h), (seqs, LANES)
            )
            av[pl.ds(h, seqs, stride=heads), :] = jnp.broadcast_to(retain_h, (seqs, LANES))

        squares = both * both
        q_sq = jnp.sum(jnp.where(low_r, squares, 0.0), axis=1, keepdims=True)
        k_sq = jnp.sum(jnp.where(low_r, 0.0, squares), axis=1, keepdims=True)
        q_dot_k = jnp.sum(jnp.where(low_r, both * swap(both), 0.0), axis=1, keepdims=True)
        q_scale = lax.rsqrt(q_sq + 1e-06) * hd ** (-0.5)
        k_scale = lax.rsqrt(k_sq + 1e-06)
        q_read = accq[...]
        q_read = q_read + swap(q_read)
        k_read = acck[...]
        k_read = (k_read + swap(k_read)) * k_scale
        retain = av[...]

        values = projected(2)
        gates = projected(3)
        to_rows(vg, values, gates)
        vgr = vg[...]
        vgs = swap(vgr)
        v2 = jnp.where(low_r, vgr, vgs)
        g2 = jnp.where(low_r, vgs, vgr)
        write = bt[...] * k_scale * (v2 - retain * k_read)
        wv[...] = write
        o = q_scale * (retain * q_read + q_dot_k * write)
        mean_sq = jnp.sum(o * o, axis=1, keepdims=True) / LANES
        g_row = gain_all[layer : layer + 1, :]
        g_row = jnp.concatenate([g_row, g_row], axis=1)
        rd[...] = o * lax.rsqrt(mean_sq + 1e-05) * g_row * (g2 * jax.nn.sigmoid(g2))
        for t in range(heads // 2):
            even = rd[pl.ds(2 * t, seqs, stride=heads), :]
            odd = rd[pl.ds(2 * t + 1, seqs, stride=heads), :]
            rall[layer, mine, t * LANES : (t + 1) * LANES] = jnp.where(low, even, odd).astype(BF16)

        gathered = []
        for i in range(1, n_dp):
            gathered.append(
                remote(
                    rall.at[layer, mine],
                    rall.at[layer, mine],
                    r_ss.at[layer, i - 1],
                    r_rs.at[layer, i - 1],
                    "dp",
                    lax.rem(me_dp + i, n_dp),
                )
            )

        def update(s, carry):
            at = pl.ds(pl.multiple_of(s * heads, heads), heads)
            keep = av[at, :]
            add = wv[at, :]
            for t in range(tiles):
                sl = slice(t * LANES, (t + 1) * LANES)
                key_t = qkx[at, flat + t * LANES : flat + (t + 1) * LANES]
                st[layer, s, :, sl] = keep * st[layer, s, :, sl] + key_t * add
            return carry

        lax.fori_loop(0, seqs, update, 0)

        loads["o", layer].wait()
        for copy in gathered:
            copy.wait_recv()
        store = pltpu.make_async_copy(st.at[layer], state_out.at[layer], out_sem.at[layer])
        store.start()
        loads["store", layer] = store
        msend[layer] = jnp.dot(rall[layer], wo[layer], preferred_element_type=F32).astype(BF16)
        mixed = []
        for i in range(1, n_tp):
            peer = lax.rem(me_tp + i, n_tp)
            mixed.append(
                remote(
                    msend.at[layer, pl.ds(pl.multiple_of(peer * share, share), share)],
                    mrecv.at[layer, i - 1],
                    m_ss.at[layer, i - 1],
                    m_rs.at[layer, i - 1],
                    "tp",
                    peer,
                )
            )
        part_rows = pl.ds(pl.multiple_of(me_tp * share, share), share)
        combined = residual_scale * stream[layer, part_rows, :].astype(F32)
        combined = combined + msend[layer, part_rows, :].astype(F32)
        for i, copy in enumerate(mixed):
            copy.wait_recv()
            combined = combined + mrecv[layer, i].astype(F32)
        s1 = jnp.sum(combined, axis=1, keepdims=True)
        s2 = jnp.sum(combined * combined, axis=1, keepdims=True)
        lane_s = lax.broadcasted_iota(jnp.int32, (share, LANES), 1)
        sums = jnp.where(lane_s < hd, s1, s2)
        ssend[layer] = sums
        stats = []
        for i in range(1, n_dp):
            stats.append(
                remote(
                    ssend.at[layer],
                    srecv.at[layer, i - 1],
                    s_ss.at[layer, i - 1],
                    s_rs.at[layer, i - 1],
                    "dp",
                    lax.rem(me_dp + i, n_dp),
                )
            )
        for i, copy in enumerate(stats):
            copy.wait_recv()
            sums = sums + srecv[layer, i]
        sums = sums / (feat * n_dp)
        mean = sums[:, 0:1]
        var = sums[:, hd : hd + 1] - mean * mean
        normed = (combined - mean) * lax.rsqrt(var + 1e-05)
        normed = normed * post_gain[layer : layer + 1, :] + post_bias[layer : layer + 1, :]
        stream[layer + 1, part_rows, :] = normed.astype(BF16)
        spread = []
        for i in range(1, n_tp):
            spread.append(
                remote(
                    stream.at[layer + 1, part_rows],
                    stream.at[layer + 1, part_rows],
                    g_ss.at[layer, i - 1],
                    g_rs.at[layer, i - 1],
                    "tp",
                    lax.rem(me_tp + i, n_tp),
                )
            )
        for copy in spread:
            copy.wait_recv()

    hidden_out[...] = stream[layers]
    for copy in sends:
        copy.wait_send()
    for layer in range(layers):
        loads["store", layer].wait()


def fused_device(n_dp, n_tp, *args):
    hidden, state, w_query = args[:3]
    w_beta, out_weight = args[6], args[10]
    layers, seqs, heads, flat = state.shape
    rows, feat = hidden.shape
    cols = w_query.shape[2]
    all_heads = w_beta.shape[2]
    share = rows // n_tp
    r = seqs * heads
    vm = pltpu.VMEM
    dma = pltpu.SemaphoreType.DMA
    whole = pl.BlockSpec(memory_space=pltpu.VMEM)
    hbm = pl.BlockSpec(memory_space=pl.ANY)
    row_tile = vm((r, LANES), F32)
    return pl.pallas_call(
        functools.partial(fused_kernel, n_dp, n_tp),
        out_shape=(
            jax.ShapeDtypeStruct(hidden.shape, BF16),
            jax.ShapeDtypeStruct(state.shape, F32),
        ),
        in_specs=[hbm] * 8
        + [pl.BlockSpec(memory_space=pltpu.SMEM), whole, hbm, whole, whole],
        out_specs=(whole, hbm),
        scratch_shapes=[
            vm((layers + 1, rows, feat), BF16),
            vm(state.shape, F32),
            vm((layers, 4, feat, cols), BF16),
            vm((layers, 2, feat, all_heads), BF16),
            vm((layers, cols, feat), BF16),
            vm((layers, 4, rows, cols), BF16),
            vm((layers, 4, n_dp - 1, seqs, cols), BF16),
            vm((layers, rows, LANES), BF16),
            vm((layers, n_dp - 1, seqs, LANES), BF16),
            vm((LANES, 2 * flat), BF16),
            vm((r, 2 * flat), F32),
        ]
        + [row_tile] * 9
        + [
            vm((layers, rows, cols), BF16),
            vm((layers, rows, feat), BF16),
            vm((layers, n_tp - 1, share, feat), BF16),
            vm((layers, share, LANES), F32),
            vm((layers, n_dp - 1, share, LANES), F32),
            dma((layers, 9)),
            dma((layers,)),
            dma((layers, 5, n_dp - 1)),
            dma((layers, 5, n_dp - 1)),
            dma((layers, n_dp - 1)),
            dma((layers, n_dp - 1)),
            dma((layers, n_tp - 1)),
            dma((layers, n_tp - 1)),
            dma((layers, n_dp - 1)),
            dma((layers, n_dp - 1)),
            dma((layers, n_tp - 1)),
            dma((layers, n_tp - 1)),
        ],
        compiler_params=pltpu.CompilerParams(
            collective_id=0, has_side_effects=True, vmem_limit_bytes=56 * 1024 * 1024
        ),
    )(*args)


def solution(mesh):
    n_dp, n_tp = mesh.shape["dp"], mesh.shape["tp"]

    def body(*args):
        hidden, state = args[:2]
        heads = state.shape[2]
        share = hidden.shape[0] // n_tp
        if heads % 8 or share % 16 or state.shape[1] % 16 or hidden.shape[1] % LANES:
            return per_device(*args)
        return fused_device(n_dp, n_tp, *args)

    placed = (
        P("grp", "dp"),
        P(None, ("grp", "dp"), "tp", None),
        P(None, "dp", "tp"),
        P(None, "dp", "tp"),
        P(None, "dp", "tp"),
        P(None, "dp", "tp"),
        P(None, "dp", None),
        P(None, "dp", None),
        P(None, "tp"),
        P(),
        P(None, "tp", "dp"),
        P(None, "dp"),
        P(None, "dp"),
    )
    return jax.shard_map(
        body,
        mesh=mesh,
        in_specs=placed,
        out_specs=(P("grp", "dp"), P(None, ("grp", "dp"), "tp", None)),
        check_vma=False,
    )
```

```python
import functools
import math

import jax
import jax.numpy as jnp
from jax import lax
from jax.experimental import pallas as pl
from jax.experimental.pallas import tpu as pltpu
from jax.sharding import PartitionSpec as P

D = 4096
HEAD_DIM = 64
LAYERS = 2


residual_scale = 2.0**0.5


def unit_norm(tensor):
    return tensor * lax.rsqrt(jnp.sum(tensor * tensor, axis=-1, keepdims=True) + 1e-06)


def delta_step(
    state_now, query_pre, key_pre, value_pre, gate_pre, beta_pre, decay_pre, decay_speed, norm_gain
):
    head_dim = query_pre.shape[-1]
    query_unit = unit_norm(query_pre.astype(jnp.float32)) * head_dim ** (-0.5)
    key_unit = unit_norm(key_pre.astype(jnp.float32))
    values_f = value_pre.astype(jnp.float32)
    beta_gate = jax.nn.sigmoid(beta_pre.astype(jnp.float32))[..., None, None]
    retain = jnp.exp(-decay_speed * jax.nn.softplus(decay_pre.astype(jnp.float32)))[..., None, None]
    matrix = state_now.reshape(state_now.shape[0], state_now.shape[1], head_dim, head_dim)
    readout = jnp.einsum("bhd,bhde->bhe", key_unit, matrix, precision=lax.Precision.HIGHEST)
    matrix = (
        retain * (matrix - beta_gate * key_unit[..., :, None] * readout[..., None, :])
        + beta_gate * key_unit[..., :, None] * values_f[..., None, :]
    )
    output_vec = jnp.einsum("bhd,bhde->bhe", query_unit, matrix, precision=lax.Precision.HIGHEST)
    output_vec = output_vec * lax.rsqrt(
        jnp.mean(output_vec * output_vec, axis=-1, keepdims=True) + 1e-05
    )
    output_vec = output_vec * norm_gain * jax.nn.silu(gate_pre.astype(jnp.float32))
    return (matrix.reshape(state_now.shape), output_vec.astype(jnp.bfloat16))


def layer_norm(combined, totals, gain_row, bias_row):
    mean_row = (totals[0] / D)[:, None]
    var_row = (totals[1] / D)[:, None] - mean_row * mean_row
    normed = (combined - mean_row) * lax.rsqrt(var_row + 1e-05)
    return (normed * gain_row + bias_row).astype(jnp.bfloat16)


def per_device(
    hidden_in,
    state_in,
    w_query,
    w_key,
    w_value,
    w_gate,
    w_beta,
    w_decay,
    decay_rate,
    out_gain,
    w_out,
    post_gain,
    post_bias,
):
    stream = hidden_in
    states = []
    heads_here = w_query.shape[2] // HEAD_DIM
    first_head = lax.axis_index("tp") * heads_here
    for block_index in range(LAYERS):
        beta_cols = lax.dynamic_slice_in_dim(w_beta[block_index], first_head, heads_here, 1)
        decay_cols = lax.dynamic_slice_in_dim(w_decay[block_index], first_head, heads_here, 1)
        part_query = jnp.dot(stream, w_query[block_index], preferred_element_type=jnp.float32)
        part_key = jnp.dot(stream, w_key[block_index], preferred_element_type=jnp.float32)
        part_value = jnp.dot(stream, w_value[block_index], preferred_element_type=jnp.float32)
        part_gate = jnp.dot(stream, w_gate[block_index], preferred_element_type=jnp.float32)
        part_beta = jnp.dot(stream, beta_cols, preferred_element_type=jnp.float32)
        part_decay = jnp.dot(stream, decay_cols, preferred_element_type=jnp.float32)
        projected = (
            lax.psum_scatter(
                part_query.astype(jnp.bfloat16), "dp", scatter_dimension=0, tiled=True
            ).astype(jnp.float32),
            lax.psum_scatter(
                part_key.astype(jnp.bfloat16), "dp", scatter_dimension=0, tiled=True
            ).astype(jnp.float32),
            lax.psum_scatter(
                part_value.astype(jnp.bfloat16), "dp", scatter_dimension=0, tiled=True
            ).astype(jnp.float32),
            lax.psum_scatter(
                part_gate.astype(jnp.bfloat16), "dp", scatter_dimension=0, tiled=True
            ).astype(jnp.float32),
            lax.psum_scatter(
                part_beta.astype(jnp.bfloat16), "dp", scatter_dimension=0, tiled=True
            ).astype(jnp.float32),
            lax.psum_scatter(
                part_decay.astype(jnp.bfloat16), "dp", scatter_dimension=0, tiled=True
            ).astype(jnp.float32),
        )
        local_rows = projected[0].shape[0]
        shaped = (local_rows, heads_here, HEAD_DIM)
        query_pre = projected[0].astype(jnp.bfloat16).reshape(shaped)
        key_pre = projected[1].astype(jnp.bfloat16).reshape(shaped)
        value_pre = projected[2].astype(jnp.bfloat16).reshape(shaped)
        gate_pre = projected[3].astype(jnp.bfloat16).reshape(shaped)
        beta_pre = projected[4].astype(jnp.bfloat16)
        decay_pre = projected[5].astype(jnp.bfloat16)
        new_state, read_vec = delta_step(
            state_in[block_index],
            query_pre,
            key_pre,
            value_pre,
            gate_pre,
            beta_pre,
            decay_pre,
            decay_rate[block_index][None, :],
            out_gain[block_index],
        )
        states.append(new_state)
        read_flat = read_vec.reshape(local_rows, heads_here * HEAD_DIM)
        out_weight = w_out[block_index]
        gathered = lax.all_gather(read_flat, "dp", axis=0, tiled=True)
        share_rows = gathered.shape[0] // lax.axis_size("tp")
        mixed_sum = lax.psum_scatter(
            jnp.dot(gathered, out_weight, preferred_element_type=jnp.float32).astype(jnp.bfloat16),
            "tp",
            scatter_dimension=0,
            tiled=True,
        ).astype(jnp.float32)
        residual = lax.dynamic_slice_in_dim(
            stream, lax.axis_index("tp") * share_rows, share_rows, 0
        )
        combined = residual_scale * residual.astype(jnp.float32) + mixed_sum
        totals = lax.psum((jnp.sum(combined, axis=1), jnp.sum(combined * combined, axis=1)), "dp")
        normed_rows = layer_norm(combined, totals, post_gain[block_index], post_bias[block_index])
        stream = lax.all_gather(normed_rows, "tp", axis=0, tiled=True)
    return (stream, jnp.stack(states, axis=0))

MESH = pl.DeviceIdType.MESH
LANES = 128
VMEM_BYTES = 67043328
VMEM_SLACK = 16 * 1024
F32 = jnp.float32
BF16 = jnp.bfloat16


def fused_kernel(
    n_dp,
    n_tp,
    hidden,
    state,
    w_query,
    w_key,
    w_value,
    w_gate,
    w_beta,
    w_decay,
    rate_in,
    gain_in,
    w_out,
    post_gain_in,
    post_bias_in,
    hidden_out,
    st,
    stream,
    wp,
    wbd,
    wo,
    psend,
    precv,
    bsend,
    brecv,
    ex,
    qkx,
    qk,
    vg,
    bt,
    dc,
    accq,
    acck,
    av,
    wv,
    rd,
    rall,
    msend,
    mrecv,
    raw,
    sums,
    rate,
    gain,
    post_gain,
    post_bias,
    load_sem,
    p_ss,
    p_rs,
    r_ss,
    r_rs,
    m_ss,
    m_rs,
    s_ss,
    s_rs,
    g_ss,
    g_rs,
):
    layers, seqs, heads, flat = st.shape
    rows, feat = stream.shape[1:]
    cols = wo.shape[1]
    share = rows // n_tp
    all_heads = wbd.shape[2]
    hd = HEAD_DIM
    tiles = flat // LANES
    me_dp = lax.axis_index("dp")
    me_tp = lax.axis_index("tp")

    loads = {}

    def load(name, src, dst, layer, index):
        copy = pltpu.make_async_copy(src, dst, load_sem.at[layer, index])
        copy.start()
        loads[name, layer] = copy

    first = pltpu.make_async_copy(hidden, stream.at[0], load_sem.at[0, 8])
    first.start()
    projections = (w_key, w_query, w_value, w_gate)

    def load_projections(layer):
        for j, w in enumerate(projections):
            load(j, w.at[layer], wp.at[layer, j], layer, j)
        load("b", w_beta.at[layer], wbd.at[layer, 0], layer, 4)
        load("d", w_decay.at[layer], wbd.at[layer, 1], layer, 5)

    def load_rest(layer):
        load("s", state.at[layer], st.at[layer], layer, 6)
        load("o", w_out.at[layer], wo.at[layer], layer, 7)

    load_projections(0)
    small = []
    for n, (src, dst) in enumerate(
        (
            (rate_in, rate),
            (gain_in, gain),
            (post_gain_in, post_gain),
            (post_bias_in, post_bias),
        )
    ):
        small.append(pltpu.make_async_copy(src, dst, load_sem.at[0, 9 + n]))
        small[-1].start()

    barrier = pltpu.get_barrier_semaphore()
    everyone = [(i, j) for i in range(n_tp) for j in range(n_dp) if i or j]

    def peer_of(i, j):
        return {"tp": lax.rem(me_tp + i, n_tp), "dp": lax.rem(me_dp + j, n_dp)}

    for i, j in everyone:
        pl.semaphore_signal(barrier, inc=1, device_id=peer_of(i, j), device_id_type=MESH)

    chunk = 1024

    def fill(n, carry):
        at = pl.multiple_of(n * chunk, chunk)
        row = lax.broadcasted_iota(jnp.int32, (LANES, chunk), 0)
        col = lax.broadcasted_iota(jnp.int32, (LANES, chunk), 1) + at
        hit = jnp.logical_and(col >= row * hd, col < (row + 1) * hd)
        ex[:, pl.ds(at, chunk)] = jnp.where(hit, 1.0, 0.0).astype(BF16)
        return carry

    lax.fori_loop(0, 2 * flat // chunk, fill, 0)
    pl.semaphore_wait(barrier, len(everyone))

    lane = lax.broadcasted_iota(jnp.int32, (seqs, LANES), 1)
    low = lane < hd
    lane_r = lax.broadcasted_iota(jnp.int32, (seqs * heads, LANES), 1)
    low_r = lane_r < hd

    def dot_t(a, b):
        return lax.dot_general(a, b, (((1,), (1,)), ((), ())), preferred_element_type=F32)

    def swap(x):
        return pltpu.roll(x, hd, 1)

    def to_rows(dst, a, b):
        for h in range(heads):
            sl = slice(h // 2 * LANES, h // 2 * LANES + LANES)
            at, bt_ = a[:, sl], b[:, sl]
            both = jnp.where(low, at, swap(bt_)) if h % 2 == 0 else jnp.where(low, swap(at), bt_)
            dst[pl.ds(h, seqs, stride=heads), :] = both

    sends = []

    def remote(src, dst, ss, rs, axis, peer, start=True):
        copy = pltpu.make_async_remote_copy(
            src_ref=src,
            dst_ref=dst,
            send_sem=ss,
            recv_sem=rs,
            device_id=peer if axis is None else {axis: peer},
            device_id_type=MESH,
        )
        if start:
            copy.start()
        sends.append(copy)
        return copy

    first.wait()
    for copy in small:
        copy.wait()
    gain_all = gain[...]
    for layer in range(layers):
        x = stream[layer]

        def scatter(group, src, dst):
            copies = []
            for i in range(1, n_dp):
                peer = lax.rem(me_dp + i, n_dp)
                copies.append(
                    remote(
                        src.at[pl.ds(pl.multiple_of(peer * seqs, seqs), seqs)],
                        dst.at[i - 1],
                        p_ss.at[layer, group, i - 1],
                        p_rs.at[layer, group, i - 1],
                        "dp",
                        peer,
                    )
                )
            return copies

        mine = pl.ds(pl.multiple_of(me_dp * seqs, seqs), seqs)
        scattered = []
        for j in range(4):
            loads[j, layer].wait()
            part = jnp.dot(x, wp[layer, j], preferred_element_type=F32)
            psend[layer, j] = part.astype(BF16)
            scattered.append(scatter(j, psend.at[layer, j], precv.at[layer, j]))
            if j == 1:
                loads["b", layer].wait()
                loads["d", layer].wait()
                pb = dot_t(x, wbd[layer, 0])
                pd = dot_t(x, wbd[layer, 1])
                pad = jnp.zeros((rows, LANES - 2 * all_heads), F32)
                bsend[layer] = jnp.concatenate([pb, pd, pad], axis=1).astype(BF16)
                scattered_b = scatter(4, bsend.at[layer], brecv.at[layer])
        load_rest(layer)
        if layer + 1 < layers:
            load_projections(layer + 1)

        def total(copies, own, got):
            acc = own.astype(F32)
            for i, copy in enumerate(copies):
                copy.wait_recv()
                acc = acc + got[i].astype(F32)
            return acc.astype(BF16).astype(F32)

        def projected(j):
            return total(scattered[j], psend[layer, j, mine, :], precv.at[layer, j])

        keys = projected(0)
        queries = projected(1)
        to_rows(qk, queries, keys)
        both = qk[...]
        both_b = both.astype(BF16)

        def expand(n, carry):
            at = pl.multiple_of(n * chunk, chunk)
            qkx[:, pl.ds(at, chunk)] = jnp.dot(
                both_b, ex[:, pl.ds(at, chunk)], preferred_element_type=F32
            )
            return carry

        lax.fori_loop(0, 2 * flat // chunk, expand, 0)
        loads["s", layer].wait()

        def reduce(s, carry):
            at = pl.ds(pl.multiple_of(s * heads, heads), heads)
            q_sums = [None, None]
            k_sums = [None, None]
            for t in range(tiles):
                sl = slice(t * LANES, (t + 1) * LANES)
                value = st[layer, s, :, sl]
                qp = qkx[at, sl] * value
                kp = qkx[at, flat + t * LANES : flat + (t + 1) * LANES] * value
                p = t % 2
                q_sums[p] = qp if q_sums[p] is None else q_sums[p] + qp
                k_sums[p] = kp if k_sums[p] is None else k_sums[p] + kp
            accq[at, :] = q_sums[0] + q_sums[1]
            acck[at, :] = k_sums[0] + k_sums[1]
            return carry

        lax.fori_loop(0, seqs, reduce, 0)

        bd = total(scattered_b, bsend[layer, mine, :], brecv.at[layer])
        for h in range(heads):
            head = me_tp * heads + h
            beta_h = jnp.sum(jnp.where(lane == head, bd, 0.0), axis=1, keepdims=True)
            decay_h = jnp.sum(jnp.where(lane == head + all_heads, bd, 0.0), axis=1, keepdims=True)
            soft = jnp.maximum(decay_h, 0.0) + jnp.log1p(jnp.exp(-jnp.abs(decay_h)))
            retain_h = jnp.exp(-rate[layer, h] * soft)
            bt[pl.ds(h, seqs, stride=heads), :] = jnp.broadcast_to(
                jax.nn.sigmoid(beta_h), (seqs, LANES)
            )
            av[pl.ds(h, seqs, stride=heads), :] = jnp.broadcast_to(retain_h, (seqs, LANES))

        squares = both * both
        q_sq = jnp.sum(jnp.where(low_r, squares, 0.0), axis=1, keepdims=True)
        k_sq = jnp.sum(jnp.where(low_r, 0.0, squares), axis=1, keepdims=True)
        q_dot_k = jnp.sum(jnp.where(low_r, both * swap(both), 0.0), axis=1, keepdims=True)
        q_scale = lax.rsqrt(q_sq + 1e-06) * hd ** (-0.5)
        k_scale = lax.rsqrt(k_sq + 1e-06)
        q_read = accq[...]
        q_read = q_read + swap(q_read)
        k_read = acck[...]
        k_read = (k_read + swap(k_read)) * k_scale
        retain = av[...]

        values = projected(2)
        gates = projected(3)
        to_rows(vg, values, gates)
        vgr = vg[...]
        vgs = swap(vgr)
        v2 = jnp.where(low_r, vgr, vgs)
        g2 = jnp.where(low_r, vgs, vgr)
        write = bt[...] * k_scale * (v2 - retain * k_read)
        wv[...] = write
        o = q_scale * (retain * q_read + q_dot_k * write)
        mean_sq = jnp.sum(o * o, axis=1, keepdims=True) / LANES
        g_row = gain_all[layer : layer + 1, :]
        g_row = jnp.concatenate([g_row, g_row], axis=1)
        rd[...] = o * lax.rsqrt(mean_sq + 1e-05) * g_row * (g2 * jax.nn.sigmoid(g2))
        for t in range(heads // 2):
            even = rd[pl.ds(2 * t, seqs, stride=heads), :]
            odd = rd[pl.ds(2 * t + 1, seqs, stride=heads), :]
            rall[layer, mine, t * LANES : (t + 1) * LANES] = jnp.where(low, even, odd).astype(BF16)

        gathered = []
        for i in range(1, n_dp):
            gathered.append(
                remote(
                    rall.at[layer, mine],
                    rall.at[layer, mine],
                    r_ss.at[layer, i - 1],
                    r_rs.at[layer, i - 1],
                    "dp",
                    lax.rem(me_dp + i, n_dp),
                )
            )

        def update(s, carry):
            at = pl.ds(pl.multiple_of(s * heads, heads), heads)
            keep = av[at, :]
            add = wv[at, :]
            for t in range(tiles):
                sl = slice(t * LANES, (t + 1) * LANES)
                key_t = qkx[at, flat + t * LANES : flat + (t + 1) * LANES]
                st[layer, s, :, sl] = keep * st[layer, s, :, sl] + key_t * add
            return carry

        lax.fori_loop(0, seqs, update, 0)

        loads["o", layer].wait()
        mixed = []
        for i in range(1, n_tp):
            peer = lax.rem(me_tp + i, n_tp)
            mixed.append(
                remote(
                    msend.at[layer, pl.ds(pl.multiple_of(peer * share, share), share)],
                    mrecv.at[layer, i - 1],
                    m_ss.at[layer, i - 1],
                    m_rs.at[layer, i - 1],
                    "tp",
                    peer,
                    start=False,
                )
            )
        for i in [0, 1] + list(range(n_dp - 1, 1, -1)):
            block = lax.rem(me_dp + n_dp - i, n_dp)
            if i:
                gathered[i - 1].wait_recv()
            at = pl.ds(pl.multiple_of(block * share, share), share)
            msend[layer, at, :] = jnp.dot(
                rall[layer, at, :], wo[layer], preferred_element_type=F32
            ).astype(BF16)
            step = lax.rem(block - me_tp + n_tp, n_tp)

            @pl.when(step > 0)
            def _():
                pltpu.make_async_remote_copy(
                    src_ref=msend.at[layer, at],
                    dst_ref=mrecv.at[layer, step - 1],
                    send_sem=m_ss.at[layer, step - 1],
                    recv_sem=m_rs.at[layer, step - 1],
                    device_id={"tp": block},
                    device_id_type=MESH,
                ).start()

        part_rows = pl.ds(pl.multiple_of(me_tp * share, share), share)
        combined = residual_scale * stream[layer, part_rows, :].astype(F32)
        combined = combined + msend[layer, part_rows, :].astype(F32)
        for i, copy in enumerate(mixed):
            copy.wait_recv()
            combined = combined + mrecv[layer, i].astype(F32)
        eye = lax.broadcasted_iota(jnp.int32, (share, LANES), 0) == lax.broadcasted_iota(
            jnp.int32, (share, LANES), 1
        )

        def as_row(column):
            return jnp.sum(jnp.where(eye, column, 0.0), axis=0, keepdims=True)

        def as_column(row):
            return jnp.sum(jnp.where(eye, row, 0.0), axis=1, keepdims=True)

        s1 = jnp.sum(combined, axis=1, keepdims=True)
        s2 = jnp.sum(combined * combined, axis=1, keepdims=True)
        sums[layer, me_tp, me_dp, 0:1, :] = as_row(s1)
        sums[layer, me_tp, me_dp, 1:2, :] = as_row(s2)
        stats = {}
        for i, j in everyone:
            stats[i, j] = remote(
                sums.at[layer, me_tp, me_dp],
                sums.at[layer, me_tp, me_dp],
                s_ss.at[layer, i, j],
                s_rs.at[layer, i, j],
                None,
                peer_of(i, j),
            )
        raw[layer, part_rows, :] = combined.astype(BF16)
        spread = []
        for i in range(1, n_tp):
            spread.append(
                remote(
                    raw.at[layer, part_rows],
                    raw.at[layer, part_rows],
                    g_ss.at[layer, i - 1],
                    g_rs.at[layer, i - 1],
                    "tp",
                    lax.rem(me_tp + i, n_tp),
                )
            )
        for copy in stats.values():
            copy.wait_recv()
        for copy in spread:
            copy.wait_recv()
        g_row = post_gain[layer : layer + 1, :]
        b_row = post_bias[layer : layer + 1, :]
        for t in range(n_tp):
            both_sums = sums[layer, t, 0]
            for d in range(1, n_dp):
                both_sums = both_sums + sums[layer, t, d]
            both_sums = both_sums / (feat * n_dp)
            mean_row = both_sums[0:1, :]
            rstd_row = lax.rsqrt(both_sums[1:2, :] - mean_row * mean_row + 1e-05)
            at = slice(t * share, (t + 1) * share)
            normed = (raw[layer, at, :].astype(F32) - as_column(mean_row)) * as_column(rstd_row)
            stream[layer + 1, at, :] = (normed * g_row + b_row).astype(BF16)

    hidden_out[...] = stream[layers]
    for copy in sends:
        copy.wait_send()


def drain_kernel(hidden, state, hidden_out, state_out, sem):
    copies = [pltpu.make_async_copy(hidden, hidden_out, sem.at[0])]
    for layer in range(state.shape[0]):
        copies.append(
            pltpu.make_async_copy(state.at[layer], state_out.at[layer], sem.at[layer + 1])
        )
    for copy in copies:
        copy.start()
    for copy in copies:
        copy.wait()


def fused_device(n_dp, n_tp, *args):
    hidden, state, w_query = args[:3]
    layers, seqs, heads, flat = state.shape
    rows, feat = hidden.shape
    cols = w_query.shape[2]
    all_heads = args[6].shape[2]
    args = args[:6] + (args[6].swapaxes(1, 2), args[7].swapaxes(1, 2)) + args[8:]
    share = rows // n_tp
    r = seqs * heads
    vm = pltpu.VMEM
    dma = pltpu.SemaphoreType.DMA
    whole = pl.BlockSpec(memory_space=pltpu.VMEM)
    hbm = pl.BlockSpec(memory_space=pl.ANY)
    grant = VMEM_BYTES - 4 * math.prod(state.shape) - 2 * math.prod(hidden.shape) - VMEM_SLACK
    row_tile = vm((r, LANES), F32)
    done = pl.pallas_call(
        functools.partial(fused_kernel, n_dp, n_tp),
        out_shape=(vm(hidden.shape, BF16), vm(state.shape, F32)),
        in_specs=[hbm] * 13,
        out_specs=(whole, whole),
        scratch_shapes=[
            vm((layers + 1, rows, feat), BF16),
            vm((layers, 4, feat, cols), BF16),
            vm((layers, 2, all_heads, feat), BF16),
            vm((layers, cols, feat), BF16),
            vm((layers, 4, rows, cols), BF16),
            vm((layers, 4, n_dp - 1, seqs, cols), BF16),
            vm((layers, rows, LANES), BF16),
            vm((layers, n_dp - 1, seqs, LANES), BF16),
            vm((LANES, 2 * flat), BF16),
            vm((r, 2 * flat), F32),
        ]
        + [row_tile] * 9
        + [
            vm((layers, rows, cols), BF16),
            vm((layers, rows, feat), BF16),
            vm((layers, n_tp - 1, share, feat), BF16),
            vm((layers, rows, feat), BF16),
            vm((layers, n_tp, n_dp, 2, LANES), F32),
            pltpu.SMEM(args[8].shape, F32),
            vm(args[9].shape, F32),
            vm(args[11].shape, F32),
            vm(args[12].shape, F32),
            dma((layers, 13)),
            dma((layers, 5, n_dp - 1)),
            dma((layers, 5, n_dp - 1)),
            dma((layers, n_dp - 1)),
            dma((layers, n_dp - 1)),
            dma((layers, n_tp - 1)),
            dma((layers, n_tp - 1)),
            dma((layers, n_tp, n_dp)),
            dma((layers, n_tp, n_dp)),
            dma((layers, n_tp - 1)),
            dma((layers, n_tp - 1)),
        ],
        compiler_params=pltpu.CompilerParams(
            collective_id=0, has_side_effects=True, vmem_limit_bytes=grant
        ),
    )(*args)
    return pl.pallas_call(
        drain_kernel,
        out_shape=(
            jax.ShapeDtypeStruct(hidden.shape, BF16),
            jax.ShapeDtypeStruct(state.shape, F32),
        ),
        in_specs=[whole, whole],
        out_specs=(hbm, hbm),
        scratch_shapes=[dma((layers + 1,))],
        compiler_params=pltpu.CompilerParams(vmem_limit_bytes=1024 * 1024),
    )(*done)


def solution(mesh):
    n_dp, n_tp = mesh.shape["dp"], mesh.shape["tp"]

    def body(*args):
        hidden, state = args[:2]
        heads = state.shape[2]
        share = hidden.shape[0] // n_tp
        if n_dp != n_tp or heads % 8 or share % 16 or state.shape[1] % 16 or hidden.shape[1] % LANES:
            return per_device(*args)
        return fused_device(n_dp, n_tp, *args)

    placed = (
        P("grp", "dp"),
        P(None, ("grp", "dp"), "tp", None),
        P(None, "dp", "tp"),
        P(None, "dp", "tp"),
        P(None, "dp", "tp"),
        P(None, "dp", "tp"),
        P(None, "dp", None),
        P(None, "dp", None),
        P(None, "tp"),
        P(),
        P(None, "tp", "dp"),
        P(None, "dp"),
        P(None, "dp"),
    )
    return jax.shard_map(
        body,
        mesh=mesh,
        in_specs=placed,
        out_specs=(P("grp", "dp"), P(None, ("grp", "dp"), "tp", None)),
        check_vma=False,
    )
```

```python
import functools
import math

import jax
import jax.numpy as jnp
from jax import lax
from jax.experimental import pallas as pl
from jax.experimental.pallas import tpu as pltpu
from jax.sharding import PartitionSpec as P

D = 4096
HEAD_DIM = 64
LAYERS = 2


residual_scale = 2.0**0.5


def unit_norm(tensor):
    return tensor * lax.rsqrt(jnp.sum(tensor * tensor, axis=-1, keepdims=True) + 1e-06)


def delta_step(
    state_now, query_pre, key_pre, value_pre, gate_pre, beta_pre, decay_pre, decay_speed, norm_gain
):
    head_dim = query_pre.shape[-1]
    query_unit = unit_norm(query_pre.astype(jnp.float32)) * head_dim ** (-0.5)
    key_unit = unit_norm(key_pre.astype(jnp.float32))
    values_f = value_pre.astype(jnp.float32)
    beta_gate = jax.nn.sigmoid(beta_pre.astype(jnp.float32))[..., None, None]
    retain = jnp.exp(-decay_speed * jax.nn.softplus(decay_pre.astype(jnp.float32)))[..., None, None]
    matrix = state_now.reshape(state_now.shape[0], state_now.shape[1], head_dim, head_dim)
    readout = jnp.einsum("bhd,bhde->bhe", key_unit, matrix, precision=lax.Precision.HIGHEST)
    matrix = (
        retain * (matrix - beta_gate * key_unit[..., :, None] * readout[..., None, :])
        + beta_gate * key_unit[..., :, None] * values_f[..., None, :]
    )
    output_vec = jnp.einsum("bhd,bhde->bhe", query_unit, matrix, precision=lax.Precision.HIGHEST)
    output_vec = output_vec * lax.rsqrt(
        jnp.mean(output_vec * output_vec, axis=-1, keepdims=True) + 1e-05
    )
    output_vec = output_vec * norm_gain * jax.nn.silu(gate_pre.astype(jnp.float32))
    return (matrix.reshape(state_now.shape), output_vec.astype(jnp.bfloat16))


def layer_norm(combined, totals, gain_row, bias_row):
    mean_row = (totals[0] / D)[:, None]
    var_row = (totals[1] / D)[:, None] - mean_row * mean_row
    normed = (combined - mean_row) * lax.rsqrt(var_row + 1e-05)
    return (normed * gain_row + bias_row).astype(jnp.bfloat16)


def per_device(
    hidden_in,
    state_in,
    w_query,
    w_key,
    w_value,
    w_gate,
    w_beta,
    w_decay,
    decay_rate,
    out_gain,
    w_out,
    post_gain,
    post_bias,
):
    stream = hidden_in
    states = []
    heads_here = w_query.shape[2] // HEAD_DIM
    first_head = lax.axis_index("tp") * heads_here
    for block_index in range(LAYERS):
        beta_cols = lax.dynamic_slice_in_dim(w_beta[block_index], first_head, heads_here, 1)
        decay_cols = lax.dynamic_slice_in_dim(w_decay[block_index], first_head, heads_here, 1)
        part_query = jnp.dot(stream, w_query[block_index], preferred_element_type=jnp.float32)
        part_key = jnp.dot(stream, w_key[block_index], preferred_element_type=jnp.float32)
        part_value = jnp.dot(stream, w_value[block_index], preferred_element_type=jnp.float32)
        part_gate = jnp.dot(stream, w_gate[block_index], preferred_element_type=jnp.float32)
        part_beta = jnp.dot(stream, beta_cols, preferred_element_type=jnp.float32)
        part_decay = jnp.dot(stream, decay_cols, preferred_element_type=jnp.float32)
        projected = (
            lax.psum_scatter(
                part_query.astype(jnp.bfloat16), "dp", scatter_dimension=0, tiled=True
            ).astype(jnp.float32),
            lax.psum_scatter(
                part_key.astype(jnp.bfloat16), "dp", scatter_dimension=0, tiled=True
            ).astype(jnp.float32),
            lax.psum_scatter(
                part_value.astype(jnp.bfloat16), "dp", scatter_dimension=0, tiled=True
            ).astype(jnp.float32),
            lax.psum_scatter(
                part_gate.astype(jnp.bfloat16), "dp", scatter_dimension=0, tiled=True
            ).astype(jnp.float32),
            lax.psum_scatter(
                part_beta.astype(jnp.bfloat16), "dp", scatter_dimension=0, tiled=True
            ).astype(jnp.float32),
            lax.psum_scatter(
                part_decay.astype(jnp.bfloat16), "dp", scatter_dimension=0, tiled=True
            ).astype(jnp.float32),
        )
        local_rows = projected[0].shape[0]
        shaped = (local_rows, heads_here, HEAD_DIM)
        query_pre = projected[0].astype(jnp.bfloat16).reshape(shaped)
        key_pre = projected[1].astype(jnp.bfloat16).reshape(shaped)
        value_pre = projected[2].astype(jnp.bfloat16).reshape(shaped)
        gate_pre = projected[3].astype(jnp.bfloat16).reshape(shaped)
        beta_pre = projected[4].astype(jnp.bfloat16)
        decay_pre = projected[5].astype(jnp.bfloat16)
        new_state, read_vec = delta_step(
            state_in[block_index],
            query_pre,
            key_pre,
            value_pre,
            gate_pre,
            beta_pre,
            decay_pre,
            decay_rate[block_index][None, :],
            out_gain[block_index],
        )
        states.append(new_state)
        read_flat = read_vec.reshape(local_rows, heads_here * HEAD_DIM)
        out_weight = w_out[block_index]
        gathered = lax.all_gather(read_flat, "dp", axis=0, tiled=True)
        share_rows = gathered.shape[0] // lax.axis_size("tp")
        mixed_sum = lax.psum_scatter(
            jnp.dot(gathered, out_weight, preferred_element_type=jnp.float32).astype(jnp.bfloat16),
            "tp",
            scatter_dimension=0,
            tiled=True,
        ).astype(jnp.float32)
        residual = lax.dynamic_slice_in_dim(
            stream, lax.axis_index("tp") * share_rows, share_rows, 0
        )
        combined = residual_scale * residual.astype(jnp.float32) + mixed_sum
        totals = lax.psum((jnp.sum(combined, axis=1), jnp.sum(combined * combined, axis=1)), "dp")
        normed_rows = layer_norm(combined, totals, post_gain[block_index], post_bias[block_index])
        stream = lax.all_gather(normed_rows, "tp", axis=0, tiled=True)
    return (stream, jnp.stack(states, axis=0))

MESH = pl.DeviceIdType.MESH
LANES = 128
VMEM_BYTES = 67043328
HALVES = 2
START = (0, 1)
ORDER = (0, 1, 0, 1, 0, 1, 0, 1)
VMEM_SLACK = 16 * 1024
F32 = jnp.float32
BF16 = jnp.bfloat16


def fused_kernel(
    n_dp,
    n_tp,
    hidden,
    state,
    w_query,
    w_key,
    w_value,
    w_gate,
    w_beta,
    w_decay,
    rate_in,
    gain_in,
    w_out,
    post_gain_in,
    post_bias_in,
    hidden_out,
    st,
    stream,
    wp,
    wbd,
    wo,
    psend,
    precv,
    bsend,
    brecv,
    ex,
    qkx,
    qk,
    vg,
    bt,
    dc,
    accq,
    acck,
    av,
    wv,
    rd,
    rall,
    msend,
    mrecv,
    raw,
    sums,
    rate,
    gain,
    post_gain,
    post_bias,
    load_sem,
    first_sem,
    p_ss,
    p_rs,
    r_ss,
    r_rs,
    m_ss,
    m_rs,
    s_ss,
    s_rs,
    g_ss,
    g_rs,
):
    layers, all_seqs, heads, flat = st.shape
    halves, _, rows, feat = stream.shape
    seqs = all_seqs // halves
    cols = wo.shape[1]
    share = rows // n_tp
    all_heads = wbd.shape[2]
    hd = HEAD_DIM
    tiles = flat // LANES
    me_dp = lax.axis_index("dp")
    me_tp = lax.axis_index("tp")

    loads = {}

    def load(name, src, dst, layer, index):
        copy = pltpu.make_async_copy(src, dst, load_sem.at[layer, index])
        copy.start()
        loads[name, layer] = copy

    first = []
    for h in range(halves):
        for d in range(n_dp):
            first.append(
                pltpu.make_async_copy(
                    hidden.at[pl.ds(d * all_seqs + h * seqs, seqs)],
                    stream.at[h, 0, pl.ds(d * seqs, seqs)],
                    first_sem.at[h, d],
                )
            )
            first[-1].start()
    projections = (w_key, w_query, w_value, w_gate)

    def load_projections(layer):
        for j, w in enumerate(projections):
            load(j, w.at[layer], wp.at[layer, j], layer, j)
        load("b", w_beta.at[layer], wbd.at[layer, 0], layer, 4)
        load("d", w_decay.at[layer], wbd.at[layer, 1], layer, 5)

    def load_rest(layer):
        load("s", state.at[layer], st.at[layer], layer, 6)
        load("o", w_out.at[layer], wo.at[layer], layer, 7)

    load_projections(0)
    small = []
    for n, (src, dst) in enumerate(
        (
            (rate_in, rate),
            (gain_in, gain),
            (post_gain_in, post_gain),
            (post_bias_in, post_bias),
        )
    ):
        small.append(pltpu.make_async_copy(src, dst, load_sem.at[0, 9 + n]))
        small[-1].start()

    barrier = pltpu.get_barrier_semaphore()
    everyone = [(i, j) for i in range(n_tp) for j in range(n_dp) if i or j]

    def peer_of(i, j):
        return {"tp": lax.rem(me_tp + i, n_tp), "dp": lax.rem(me_dp + j, n_dp)}

    for i, j in everyone:
        pl.semaphore_signal(barrier, inc=1, device_id=peer_of(i, j), device_id_type=MESH)

    chunk = 1024

    def fill(n, carry):
        at = pl.multiple_of(n * chunk, chunk)
        row = lax.broadcasted_iota(jnp.int32, (LANES, chunk), 0)
        col = lax.broadcasted_iota(jnp.int32, (LANES, chunk), 1) + at
        hit = jnp.logical_and(col >= row * hd, col < (row + 1) * hd)
        ex[:, pl.ds(at, chunk)] = jnp.where(hit, 1.0, 0.0).astype(BF16)
        return carry

    lax.fori_loop(0, 2 * flat // chunk, fill, 0)
    pl.semaphore_wait(barrier, len(everyone))

    lane = lax.broadcasted_iota(jnp.int32, (seqs, LANES), 1)
    low = lane < hd
    lane_r = lax.broadcasted_iota(jnp.int32, (seqs * heads, LANES), 1)
    low_r = lane_r < hd

    def dot_t(a, b):
        return lax.dot_general(a, b, (((1,), (1,)), ((), ())), preferred_element_type=F32)

    def swap(x):
        return pltpu.roll(x, hd, 1)

    def to_rows(dst, a, b):
        for h in range(heads):
            sl = slice(h // 2 * LANES, h // 2 * LANES + LANES)
            at, bt_ = a[:, sl], b[:, sl]
            both = jnp.where(low, at, swap(bt_)) if h % 2 == 0 else jnp.where(low, swap(at), bt_)
            dst[pl.ds(h, seqs, stride=heads), :] = both

    sends = []

    def remote(src, dst, ss, rs, axis, peer, start=True):
        copy = pltpu.make_async_remote_copy(
            src_ref=src,
            dst_ref=dst,
            send_sem=ss,
            recv_sem=rs,
            device_id=peer if axis is None else {axis: peer},
            device_id_type=MESH,
        )
        if start:
            copy.start()
        sends.append(copy)
        return copy

    for copy in first:
        copy.wait()
    for copy in small:
        copy.wait()
    gain_all = gain[...]
    def block(layer, half):
        x = stream[half, layer]

        def scatter(group, src, dst):
            copies = []
            for i in range(1, n_dp):
                peer = lax.rem(me_dp + i, n_dp)
                copies.append(
                    remote(
                        src.at[pl.ds(pl.multiple_of(peer * seqs, seqs), seqs)],
                        dst.at[i - 1],
                        p_ss.at[half, layer, group, i - 1],
                        p_rs.at[half, layer, group, i - 1],
                        "dp",
                        peer,
                    )
                )
            return copies

        mine = pl.ds(pl.multiple_of(me_dp * seqs, seqs), seqs)
        scattered = []
        for j in range(4):
            if half == 0:
                loads[j, layer].wait()
            part = jnp.dot(x, wp[layer, j], preferred_element_type=F32)
            psend[half, layer, j] = part.astype(BF16)
            scattered.append(scatter(j, psend.at[half, layer, j], precv.at[half, layer, j]))
            if j == 1:
                if half == 0:
                    loads["b", layer].wait()
                if half == 0:
                    loads["d", layer].wait()
                pb = dot_t(x, wbd[layer, 0])
                pd = dot_t(x, wbd[layer, 1])
                pad = jnp.zeros((rows, LANES - 2 * all_heads), F32)
                bsend[half, layer] = jnp.concatenate([pb, pd, pad], axis=1).astype(BF16)
                scattered_b = scatter(4, bsend.at[half, layer], brecv.at[half, layer])
        if half == 0:
            load_rest(layer)
            if layer + 1 < layers:
                load_projections(layer + 1)
        yield

        def total(copies, own, got):
            acc = own.astype(F32)
            for i, copy in enumerate(copies):
                copy.wait_recv()
                acc = acc + got[i].astype(F32)
            return acc.astype(BF16).astype(F32)

        def projected(j):
            return total(scattered[j], psend[half, layer, j, mine, :], precv.at[half, layer, j])

        keys = projected(0)
        queries = projected(1)
        to_rows(qk, queries, keys)
        both = qk[...]
        both_b = both.astype(BF16)

        def expand(n, carry):
            at = pl.multiple_of(n * chunk, chunk)
            qkx[:, pl.ds(at, chunk)] = jnp.dot(
                both_b, ex[:, pl.ds(at, chunk)], preferred_element_type=F32
            )
            return carry

        lax.fori_loop(0, 2 * flat // chunk, expand, 0)
        if half == 0:
            loads["s", layer].wait()

        def reduce(s, carry):
            at = pl.ds(pl.multiple_of(s * heads, heads), heads)
            q_sums = [None, None]
            k_sums = [None, None]
            for t in range(tiles):
                sl = slice(t * LANES, (t + 1) * LANES)
                value = st[layer, half * seqs + s, :, sl]
                qp = qkx[at, sl] * value
                kp = qkx[at, flat + t * LANES : flat + (t + 1) * LANES] * value
                p = t % 2
                q_sums[p] = qp if q_sums[p] is None else q_sums[p] + qp
                k_sums[p] = kp if k_sums[p] is None else k_sums[p] + kp
            accq[at, :] = q_sums[0] + q_sums[1]
            acck[at, :] = k_sums[0] + k_sums[1]
            return carry

        lax.fori_loop(0, seqs, reduce, 0)

        bd = total(scattered_b, bsend[half, layer, mine, :], brecv.at[half, layer])
        for h in range(heads):
            head = me_tp * heads + h
            beta_h = jnp.sum(jnp.where(lane == head, bd, 0.0), axis=1, keepdims=True)
            decay_h = jnp.sum(jnp.where(lane == head + all_heads, bd, 0.0), axis=1, keepdims=True)
            soft = jnp.maximum(decay_h, 0.0) + jnp.log1p(jnp.exp(-jnp.abs(decay_h)))
            retain_h = jnp.exp(-rate[layer, h] * soft)
            bt[pl.ds(h, seqs, stride=heads), :] = jnp.broadcast_to(
                jax.nn.sigmoid(beta_h), (seqs, LANES)
            )
            av[pl.ds(h, seqs, stride=heads), :] = jnp.broadcast_to(retain_h, (seqs, LANES))

        squares = both * both
        q_sq = jnp.sum(jnp.where(low_r, squares, 0.0), axis=1, keepdims=True)
        k_sq = jnp.sum(jnp.where(low_r, 0.0, squares), axis=1, keepdims=True)
        q_dot_k = jnp.sum(jnp.where(low_r, both * swap(both), 0.0), axis=1, keepdims=True)
        q_scale = lax.rsqrt(q_sq + 1e-06) * hd ** (-0.5)
        k_scale = lax.rsqrt(k_sq + 1e-06)
        q_read = accq[...]
        q_read = q_read + swap(q_read)
        k_read = acck[...]
        k_read = (k_read + swap(k_read)) * k_scale
        retain = av[...]

        values = projected(2)
        gates = projected(3)
        to_rows(vg, values, gates)
        vgr = vg[...]
        vgs = swap(vgr)
        v2 = jnp.where(low_r, vgr, vgs)
        g2 = jnp.where(low_r, vgs, vgr)
        write = bt[...] * k_scale * (v2 - retain * k_read)
        wv[...] = write
        o = q_scale * (retain * q_read + q_dot_k * write)
        mean_sq = jnp.sum(o * o, axis=1, keepdims=True) / LANES
        g_row = gain_all[layer : layer + 1, :]
        g_row = jnp.concatenate([g_row, g_row], axis=1)
        rd[...] = o * lax.rsqrt(mean_sq + 1e-05) * g_row * (g2 * jax.nn.sigmoid(g2))
        for t in range(heads // 2):
            even = rd[pl.ds(2 * t, seqs, stride=heads), :]
            odd = rd[pl.ds(2 * t + 1, seqs, stride=heads), :]
            rall[half, layer, mine, t * LANES : (t + 1) * LANES] = jnp.where(low, even, odd).astype(BF16)

        gathered = []
        for i in range(1, n_dp):
            gathered.append(
                remote(
                    rall.at[half, layer, mine],
                    rall.at[half, layer, mine],
                    r_ss.at[half, layer, i - 1],
                    r_rs.at[half, layer, i - 1],
                    "dp",
                    lax.rem(me_dp + i, n_dp),
                )
            )

        def update(s, carry):
            at = pl.ds(pl.multiple_of(s * heads, heads), heads)
            keep = av[at, :]
            add = wv[at, :]
            for t in range(tiles):
                sl = slice(t * LANES, (t + 1) * LANES)
                key_t = qkx[at, flat + t * LANES : flat + (t + 1) * LANES]
                st[layer, half * seqs + s, :, sl] = keep * st[layer, half * seqs + s, :, sl] + key_t * add
            return carry

        lax.fori_loop(0, seqs, update, 0)
        yield

        if half == 0:
            loads["o", layer].wait()
        mixed = []
        for i in range(1, n_tp):
            peer = lax.rem(me_tp + i, n_tp)
            mixed.append(
                remote(
                    msend.at[half, layer, pl.ds(pl.multiple_of(peer * share, share), share)],
                    mrecv.at[half, layer, i - 1],
                    m_ss.at[half, layer, i - 1],
                    m_rs.at[half, layer, i - 1],
                    "tp",
                    peer,
                    start=False,
                )
            )
        for i in [0, 1] + list(range(n_dp - 1, 1, -1)):
            block = lax.rem(me_dp + n_dp - i, n_dp)
            if i:
                gathered[i - 1].wait_recv()
            at = pl.ds(pl.multiple_of(block * share, share), share)
            msend[half, layer, at, :] = jnp.dot(
                rall[half, layer, at, :], wo[layer], preferred_element_type=F32
            ).astype(BF16)
            step = lax.rem(block - me_tp + n_tp, n_tp)

            @pl.when(step > 0)
            def _():
                pltpu.make_async_remote_copy(
                    src_ref=msend.at[half, layer, at],
                    dst_ref=mrecv.at[half, layer, step - 1],
                    send_sem=m_ss.at[half, layer, step - 1],
                    recv_sem=m_rs.at[half, layer, step - 1],
                    device_id={"tp": block},
                    device_id_type=MESH,
                ).start()

        yield
        part_rows = pl.ds(pl.multiple_of(me_tp * share, share), share)
        combined = residual_scale * stream[half, layer, part_rows, :].astype(F32)
        combined = combined + msend[half, layer, part_rows, :].astype(F32)
        for i, copy in enumerate(mixed):
            copy.wait_recv()
            combined = combined + mrecv[half, layer, i].astype(F32)
        eye = lax.broadcasted_iota(jnp.int32, (share, LANES), 0) == lax.broadcasted_iota(
            jnp.int32, (share, LANES), 1
        )

        def as_row(column):
            return jnp.sum(jnp.where(eye, column, 0.0), axis=0, keepdims=True)

        def as_column(row):
            return jnp.sum(jnp.where(eye, row, 0.0), axis=1, keepdims=True)

        s1 = jnp.sum(combined, axis=1, keepdims=True)
        s2 = jnp.sum(combined * combined, axis=1, keepdims=True)
        sums[half, layer, me_tp, me_dp, 0:1, :] = as_row(s1)
        sums[half, layer, me_tp, me_dp, 1:2, :] = as_row(s2)
        stats = {}
        for i, j in everyone:
            stats[i, j] = remote(
                sums.at[half, layer, me_tp, me_dp],
                sums.at[half, layer, me_tp, me_dp],
                s_ss.at[half, layer, i, j],
                s_rs.at[half, layer, i, j],
                None,
                peer_of(i, j),
            )
        raw[half, layer, part_rows, :] = combined.astype(BF16)
        spread = []
        for i in range(1, n_tp):
            spread.append(
                remote(
                    raw.at[half, layer, part_rows],
                    raw.at[half, layer, part_rows],
                    g_ss.at[half, layer, i - 1],
                    g_rs.at[half, layer, i - 1],
                    "tp",
                    lax.rem(me_tp + i, n_tp),
                )
            )
        yield
        for copy in stats.values():
            copy.wait_recv()
        for copy in spread:
            copy.wait_recv()
        g_row = post_gain[layer : layer + 1, :]
        b_row = post_bias[layer : layer + 1, :]
        for t in range(n_tp):
            both_sums = sums[half, layer, t, 0]
            for d in range(1, n_dp):
                both_sums = both_sums + sums[half, layer, t, d]
            both_sums = both_sums / (feat * n_dp)
            mean_row = both_sums[0:1, :]
            rstd_row = lax.rsqrt(both_sums[1:2, :] - mean_row * mean_row + 1e-05)
            at = slice(t * share, (t + 1) * share)
            normed = (raw[half, layer, at, :].astype(F32) - as_column(mean_row)) * as_column(rstd_row)
            stream[half, layer + 1, at, :] = (normed * g_row + b_row).astype(BF16)

    def run(half):
        for layer in range(layers):
            yield from block(layer, half)

    runs = [run(half) for half in range(halves)]
    for half in START + ORDER * layers:
        next(runs[half], None)

    for h in range(halves):
        for d in range(n_dp):
            at = d * all_seqs + h * seqs
            hidden_out[at : at + seqs, :] = stream[h, layers, d * seqs : (d + 1) * seqs, :]
    for copy in sends:
        copy.wait_send()


def drain_kernel(hidden, state, hidden_out, state_out, sem):
    copies = [pltpu.make_async_copy(hidden, hidden_out, sem.at[0])]
    for layer in range(state.shape[0]):
        copies.append(
            pltpu.make_async_copy(state.at[layer], state_out.at[layer], sem.at[layer + 1])
        )
    for copy in copies:
        copy.start()
    for copy in copies:
        copy.wait()


def fused_device(n_dp, n_tp, *args):
    hidden, state, w_query = args[:3]
    layers, seqs, heads, flat = state.shape
    rows, feat = hidden.shape[0] // HALVES, hidden.shape[1]
    seqs = seqs // HALVES
    cols = w_query.shape[2]
    all_heads = args[6].shape[2]
    args = args[:6] + (args[6].swapaxes(1, 2), args[7].swapaxes(1, 2)) + args[8:]
    share = rows // n_tp
    r = seqs * heads
    vm = pltpu.VMEM
    dma = pltpu.SemaphoreType.DMA
    whole = pl.BlockSpec(memory_space=pltpu.VMEM)
    hbm = pl.BlockSpec(memory_space=pl.ANY)
    grant = VMEM_BYTES - 4 * math.prod(state.shape) - 2 * math.prod(hidden.shape) - VMEM_SLACK
    row_tile = vm((r, LANES), F32)
    done = pl.pallas_call(
        functools.partial(fused_kernel, n_dp, n_tp),
        out_shape=(vm(hidden.shape, BF16), vm(state.shape, F32)),
        in_specs=[hbm] * 13,
        out_specs=(whole, whole),
        scratch_shapes=[
            vm((HALVES, layers + 1, rows, feat), BF16),
            vm((layers, 4, feat, cols), BF16),
            vm((layers, 2, all_heads, feat), BF16),
            vm((layers, cols, feat), BF16),
            vm((HALVES, layers, 4, rows, cols), BF16),
            vm((HALVES, layers, 4, n_dp - 1, seqs, cols), BF16),
            vm((HALVES, layers, rows, LANES), BF16),
            vm((HALVES, layers, n_dp - 1, seqs, LANES), BF16),
            vm((LANES, 2 * flat), BF16),
            vm((r, 2 * flat), F32),
        ]
        + [row_tile] * 9
        + [
            vm((HALVES, layers, rows, cols), BF16),
            vm((HALVES, layers, rows, feat), BF16),
            vm((HALVES, layers, n_tp - 1, share, feat), BF16),
            vm((HALVES, layers, rows, feat), BF16),
            vm((HALVES, layers, n_tp, n_dp, 2, LANES), F32),
            pltpu.SMEM(args[8].shape, F32),
            vm(args[9].shape, F32),
            vm(args[11].shape, F32),
            vm(args[12].shape, F32),
            dma((layers, 13)),
            dma((HALVES, n_dp)),
            dma((HALVES, layers, 5, n_dp - 1)),
            dma((HALVES, layers, 5, n_dp - 1)),
            dma((HALVES, layers, n_dp - 1)),
            dma((HALVES, layers, n_dp - 1)),
            dma((HALVES, layers, n_tp - 1)),
            dma((HALVES, layers, n_tp - 1)),
            dma((HALVES, layers, n_tp, n_dp)),
            dma((HALVES, layers, n_tp, n_dp)),
            dma((HALVES, layers, n_tp - 1)),
            dma((HALVES, layers, n_tp - 1)),
        ],
        compiler_params=pltpu.CompilerParams(
            collective_id=0, has_side_effects=True, vmem_limit_bytes=grant
        ),
    )(*args)
    return pl.pallas_call(
        drain_kernel,
        out_shape=(
            jax.ShapeDtypeStruct(hidden.shape, BF16),
            jax.ShapeDtypeStruct(state.shape, F32),
        ),
        in_specs=[whole, whole],
        out_specs=(hbm, hbm),
        scratch_shapes=[dma((layers + 1,))],
        compiler_params=pltpu.CompilerParams(vmem_limit_bytes=1024 * 1024),
    )(*done)


def solution(mesh):
    n_dp, n_tp = mesh.shape["dp"], mesh.shape["tp"]

    def body(*args):
        hidden, state = args[:2]
        heads = state.shape[2]
        share = hidden.shape[0] // n_tp
        if n_dp != n_tp or heads % 8 or share % (16 * HALVES) or hidden.shape[1] % LANES:
            return per_device(*args)
        return fused_device(n_dp, n_tp, *args)

    placed = (
        P("grp", "dp"),
        P(None, ("grp", "dp"), "tp", None),
        P(None, "dp", "tp"),
        P(None, "dp", "tp"),
        P(None, "dp", "tp"),
        P(None, "dp", "tp"),
        P(None, "dp", None),
        P(None, "dp", None),
        P(None, "tp"),
        P(),
        P(None, "tp", "dp"),
        P(None, "dp"),
        P(None, "dp"),
    )
    return jax.shard_map(
        body,
        mesh=mesh,
        in_specs=placed,
        out_specs=(P("grp", "dp"), P(None, ("grp", "dp"), "tp", None)),
        check_vma=False,
    )
```
